32 devices in a mesh: sp: 8 (over z, y), tp: 4 (over x, core).
Axes of the slice: x: 2, y: 2, z: 4, core: 2. Of those that a mesh axis runs over, the one named last changes fastest.
Arguments:
- tokens: bfloat16 [3072, 4096], P(('sp', 'tp')), may hold values from -6 to 6
- norm_gain: bfloat16 [4096], replicated, may hold values from 0.099609375 to 1.8984375
- w_pool_in: bfloat16 [4096, 4096], P('sp', 'tp'), may hold values from -0.09375 to 0.09375
- w_mem_in: bfloat16 [4096, 4096], P('sp', 'tp'), may hold values from -0.09375 to 0.09375
- w_input_gate: bfloat16 [4096, 16], replicated, may hold values from -104 to 104
- w_forget_gate: bfloat16 [4096, 16], replicated, may hold values from -0.09375 to 0.09375
- forget_bias: float32 [16], replicated, may hold values from 3 to 13
- forget_extra: float32 [3072, 16], P('sp', 'tp'), may hold values from 0 to 1.5
- conv_weight: bfloat16 [4, 4096], replicated, may hold values from -3 to 3
- query_map: bfloat16 [1024, 4, 4], replicated, may hold values from -3 to 3
- key_map: bfloat16 [1024, 4, 4], replicated, may hold values from -3 to 3
- pool_map: bfloat16 [16, 256, 256], P('tp'), may hold values from -0.375 to 0.375
- pool_gain: bfloat16 [4096], replicated, may hold values from 0.099609375 to 1.8984375
- mem_gain: bfloat16 [4096], replicated, may hold values from 0.099609375 to 1.8984375
- w_out_pool: bfloat16 [4096, 4096], P('tp', 'sp'), may hold values from -0.0625 to 0.0625
- w_out_mem: bfloat16 [4096, 4096], P('tp', 'sp'), may hold values from -0.0625 to 0.0625
Outputs:
- layer_out: bfloat16 [3072, 4096], P(('sp', 'tp'))
The draws below stay inside these ranges and needn't reach their ends.
All inputs are finite; a program needn't handle non-finite values.
Results may differ from the reference program's by a relative error of at most 0.019.
The reference program's roundings to bfloat16 on the way count: a program that leaves them out, or rounds other values in their place, can miss the bound.
Values may be sent and summed in bfloat16 or wider, within the bound.
A program may use at most 128 MiB of HBM per device.

```python
import jax
import jax.numpy as jnp
from jax import lax

D = 4096
POOL = 4096
MEM = 4096
HEAD = 256
CONV = 4
BLOCK = 128
TOK_DEV = 384
MEMORY_HEADS = 16
GROUPS = 16
SEQUENCE_TOKENS = 3072
N_TP = 4


def draw_w_input_gate(key, part):
    reach_value = 3.0
    values = jax.random.uniform(jax.random.fold_in(key, 301), (D, MEMORY_HEADS), jnp.float32, -reach_value, reach_value)
    return values.astype(jnp.bfloat16)


def draw_forget_bias(key, part):
    pick_key, fast_key, slow_key = jax.random.split(jax.random.fold_in(key, 302), 3)
    slow_share = 0.5
    slow_heads = jax.random.bernoulli(pick_key, slow_share, (MEMORY_HEADS,))
    fast_value = jax.random.uniform(fast_key, (MEMORY_HEADS,), jnp.float32, 3.0, 3.8)
    slow_value = jnp.log(SEQUENCE_TOKENS * 1.0) + jax.random.uniform(slow_key, (MEMORY_HEADS,), jnp.float32, 1.5, 2.5)
    return jnp.where(slow_heads, slow_value, fast_value).astype(jnp.float32)


def draw_forget_extra(key, part):
    frequency_key, spike_key, quantity_key = jax.random.split(jax.random.fold_in(key, 303), 3)
    segments = SEQUENCE_TOKENS // TOK_DEV
    decay_rate = jnp.exp(jax.random.uniform(frequency_key, (segments, 1, MEMORY_HEADS), jnp.float32, jnp.log(0.1), jnp.log(0.8))) / SEQUENCE_TOKENS
    constant_level = jnp.broadcast_to(decay_rate, (segments, TOK_DEV, MEMORY_HEADS)).reshape(SEQUENCE_TOKENS, MEMORY_HEADS)
    spike_rows = jax.random.randint(spike_key, (2, MEMORY_HEADS), 0, SEQUENCE_TOKENS)
    quantities = -jnp.log(1.0 - jax.random.uniform(quantity_key, (2, MEMORY_HEADS), jnp.float32, 0.2, 0.5))
    location_rows = jnp.arange(SEQUENCE_TOKENS)[:, None, None] == spike_rows[None]
    spikes = jnp.sum(jnp.where(location_rows, quantities[None], 0.0), axis=1)
    return (constant_level + spikes).astype(jnp.float32)


def levels(own_key, extent, cuts, least, high):
    level, own = 1.0, jax.random.fold_in(own_key, 6)
    for axis_at, blocks in cuts:
        steps = jnp.exp(jax.random.uniform(jax.random.fold_in(own, axis_at), (blocks,), jnp.float32, least / len(cuts), high / len(cuts)))
        level = level * jnp.repeat(steps, extent[axis_at] // blocks).reshape([-1 if axis == axis_at else 1 for axis in range(len(extent))])
    return level


def bell_draw(rng, dims, deviation, bound, cuts=(), held_as=jnp.bfloat16):
    values = deviation * jax.random.normal(rng, dims, jnp.float32)
    if cuts:
        values = values * levels(rng, dims, cuts, -0.22, 0.18)
    return jnp.clip(values, -bound, bound).astype(held_as)


def setup_inputs(seed: int = 0) -> dict:
    arg_keys = jax.random.split(jax.random.key(seed), 17)
    return {
        "tokens": bell_draw(arg_keys[0], (SEQUENCE_TOKENS, D), 1.0, 6.0, ((0, 32),)),
        "norm_gain": jnp.clip(1.0 + 0.18 * jax.random.normal(arg_keys[1], (D,), jnp.float32), 0.099609375, 1.8984375).astype(jnp.bfloat16),
        "w_pool_in": bell_draw(arg_keys[2], (D, POOL), D ** -0.5, 0.09375, ((0, 8), (1, 4))),
        "w_mem_in": bell_draw(arg_keys[3], (D, MEM), D ** -0.5, 0.09375, ((0, 8), (1, 4))),
        "w_input_gate": draw_w_input_gate(jax.random.fold_in(arg_keys[16], 71), 0),
        "w_forget_gate": bell_draw(arg_keys[5], (D, MEMORY_HEADS), D ** -0.5, 0.09375),
        "forget_bias": draw_forget_bias(jax.random.fold_in(arg_keys[16], 71), 0),
        "forget_extra": draw_forget_extra(jax.random.fold_in(arg_keys[16], 71), 0),
        "conv_weight": bell_draw(arg_keys[8], (CONV, MEM), CONV ** -0.5, 3.0),
        "query_map": bell_draw(arg_keys[9], (MEM // 4, 4, 4), 4 ** -0.5, 3.0),
        "key_map": bell_draw(arg_keys[10], (MEM // 4, 4, 4), 4 ** -0.5, 3.0),
        "pool_map": bell_draw(arg_keys[11], (GROUPS, HEAD, HEAD), HEAD ** -0.5, 0.375, ((0, 4),)),
        "pool_gain": jnp.clip(1.0 + 0.18 * jax.random.normal(arg_keys[12], (POOL,), jnp.float32), 0.099609375, 1.8984375).astype(jnp.bfloat16),
        "mem_gain": jnp.clip(1.0 + 0.18 * jax.random.normal(arg_keys[13], (MEM,), jnp.float32), 0.099609375, 1.8984375).astype(jnp.bfloat16),
        "w_out_pool": bell_draw(arg_keys[14], (POOL, D), (POOL + MEM) ** -0.5, 0.0625, ((0, 4), (1, 8))),
        "w_out_mem": bell_draw(arg_keys[15], (MEM, D), (POOL + MEM) ** -0.5, 0.0625, ((0, 4), (1, 8))),
    }


epsilon = 1e-06
windows_all = (2, 4, 8, 16)
highest = lax.Precision.HIGHEST

def rms_rows(rows, gain):
    values = rows.astype(jnp.float32)
    factor = lax.rsqrt(lax.optimization_barrier(jnp.mean(values * values, axis=-1, keepdims=True)) + epsilon)
    return (values * factor * gain.astype(jnp.float32)).astype(jnp.bfloat16)

def rounded(values):
    return lax.optimization_barrier(values.astype(jnp.bfloat16)).astype(jnp.float32)

def pool_branch(pool_in, pool_map, pool_gain):
    values = pool_in.astype(jnp.float32)
    position = jnp.arange(1, SEQUENCE_TOKENS + 1).astype(jnp.float32)[:, None]
    outputs = []
    for group_index in range(GROUPS):
        window = windows_all[group_index % 4]
        columns = values[:, group_index * HEAD:(group_index + 1) * HEAD]
        padded = jnp.pad(columns, ((window, 0), (0, 0)))
        window_total = padded[window:window + SEQUENCE_TOKENS]
        for offset in range(1, window):
            window_total = window_total + padded[window - offset:window - offset + SEQUENCE_TOKENS]
        counts = jnp.minimum(position, float(window))
        centred = (window_total / counts - columns).astype(jnp.bfloat16)
        mapped = jnp.dot(centred, pool_map[group_index], preferred_element_type=jnp.float32)
        outputs.append(mapped * pool_gain[group_index * HEAD:(group_index + 1) * HEAD].astype(jnp.float32))
    return jnp.concatenate(outputs, axis=1).astype(jnp.bfloat16)

def head_memory(inputs):
    query_rows, key_rows, value_rows, input_pre, log_forget = inputs
    blocks = SEQUENCE_TOKENS // BLOCK
    causal_mask = jnp.tril(jnp.ones((BLOCK, BLOCK), dtype=jnp.bool_))
    key_scale = HEAD ** (-0.5)

    def advance(carried_state, block_part):
        memory, peak_log = carried_state
        query_now, key_now, value_now, input_now, forget_now = block_part
        cumulative = jnp.cumsum(forget_now)
        block_total = cumulative[-1]
        log_diff = jnp.where(causal_mask, cumulative[:, None] - cumulative[None, :] + input_now[None, :], -jnp.inf)
        carry_log = cumulative + peak_log
        row_peak = jnp.maximum(lax.optimization_barrier(jnp.max(log_diff, axis=1)), carry_log)
        scores = jnp.dot(query_now, key_now.T, preferred_element_type=jnp.float32) * key_scale
        block_weights = (jnp.exp(log_diff - row_peak[:, None]) * scores).astype(jnp.bfloat16)
        within_block = jnp.dot(block_weights, value_now, preferred_element_type=jnp.float32)
        carried = jnp.dot(query_now.astype(jnp.float32), memory, precision=highest)
        carried = carried * jnp.exp(carry_log - row_peak)[:, None]
        hidden = within_block + carried
        along_log = block_total - cumulative + input_now
        new_peak = jnp.maximum(block_total + peak_log, jnp.max(along_log))
        scaled_keys = key_now.astype(jnp.float32) * (jnp.exp(along_log - new_peak) * key_scale)[:, None]
        memory = jnp.exp(block_total + peak_log - new_peak) * memory + jnp.dot(scaled_keys.T, value_now.astype(jnp.float32), precision=highest)
        return ((memory, new_peak), hidden)
    initial = (jnp.zeros((HEAD, HEAD), jnp.float32), jnp.zeros((), jnp.float32))
    stacked = (query_rows.reshape(blocks, BLOCK, HEAD), key_rows.reshape(blocks, BLOCK, HEAD), value_rows.reshape(blocks, BLOCK, HEAD), input_pre.reshape(blocks, BLOCK), log_forget.reshape(blocks, BLOCK))
    unused, hidden = lax.scan(advance, initial, stacked)
    return hidden.reshape(SEQUENCE_TOKENS, HEAD)

def by_head(array):
    return jnp.swapaxes(array.reshape(SEQUENCE_TOKENS, MEMORY_HEADS, HEAD), 0, 1)

def reference(tokens, norm_gain, w_pool_in, w_mem_in, w_input_gate, w_forget_gate, forget_bias, forget_extra, conv_weight, query_map, key_map, pool_map, pool_gain, mem_gain, w_out_pool, w_out_mem):
    normalized = rms_rows(tokens, norm_gain)
    pool_in = jnp.dot(normalized, w_pool_in, preferred_element_type=jnp.float32).astype(jnp.bfloat16)
    mem_in = jnp.dot(normalized, w_mem_in, preferred_element_type=jnp.float32).astype(jnp.bfloat16)
    input_pre = rounded(jnp.dot(normalized, w_input_gate, preferred_element_type=jnp.float32) * D ** (-0.5))
    forget_pre = rounded(jnp.dot(normalized, w_forget_gate, preferred_element_type=jnp.float32))
    log_forget = jax.nn.log_sigmoid(forget_pre + forget_bias) - forget_extra
    pool_mixed = pool_branch(pool_in, pool_map, pool_gain)
    padded = jnp.pad(mem_in.astype(jnp.float32), ((CONV - 1, 0), (0, 0)))
    conv_sum = padded[0:SEQUENCE_TOKENS] * conv_weight[0].astype(jnp.float32)
    for tap_index in range(1, CONV):
        conv_sum = conv_sum + padded[tap_index:tap_index + SEQUENCE_TOKENS] * conv_weight[tap_index].astype(jnp.float32)
    conv_in = jax.nn.silu(conv_sum).astype(jnp.bfloat16)
    conv_blocks = conv_in.astype(jnp.float32).reshape(SEQUENCE_TOKENS, MEM // 4, 4)
    query_rows = jnp.einsum('tnc,ncd->tnd', conv_blocks, query_map.astype(jnp.float32)).reshape(SEQUENCE_TOKENS, MEM).astype(jnp.bfloat16)
    key_rows = jnp.einsum('tnc,ncd->tnd', conv_blocks, key_map.astype(jnp.float32)).reshape(SEQUENCE_TOKENS, MEM).astype(jnp.bfloat16)
    hidden = lax.map(head_memory, (by_head(query_rows), by_head(key_rows), by_head(mem_in), input_pre.T, log_forget.T))
    hidden = jnp.swapaxes(hidden, 0, 1)
    centre = lax.optimization_barrier(jnp.mean(hidden, axis=-1, keepdims=True))
    spread_sq = lax.optimization_barrier(jnp.mean(jnp.square(hidden - centre), axis=-1, keepdims=True))
    normed = ((hidden - centre) * lax.rsqrt(spread_sq + epsilon)).reshape(SEQUENCE_TOKENS, MEM)
    mem_mixed = (normed * mem_gain.astype(jnp.float32)).astype(jnp.bfloat16)
    pool_run = POOL // N_TP
    mem_run = MEM // N_TP
    layer_out = jnp.zeros((SEQUENCE_TOKENS, D), jnp.float32)
    for member in range(N_TP):
        run_partial = jnp.dot(pool_mixed[:, member * pool_run:(member + 1) * pool_run], w_out_pool[member * pool_run:(member + 1) * pool_run], preferred_element_type=jnp.float32)
        run_partial = run_partial + jnp.dot(mem_mixed[:, member * mem_run:(member + 1) * mem_run], w_out_mem[member * mem_run:(member + 1) * mem_run], preferred_element_type=jnp.float32)
        layer_out = layer_out + rounded(run_partial)
    return layer_out.astype(jnp.bfloat16)
```

```python
import jax
import jax.numpy as jnp
from jax import lax
from jax.sharding import PartitionSpec as P

HEAD = 256
CONV = 4
BLOCK = 128

epsilon = 1e-06
highest = lax.Precision.HIGHEST
lowest = -1e30
f32 = jnp.float32
bf16 = jnp.bfloat16


def rms_rows(rows, gain):
    values = rows.astype(f32)
    factor = lax.rsqrt(jnp.mean(values * values, axis=-1, keepdims=True) + epsilon)
    return (values * factor * gain.astype(f32)).astype(bf16)


def swap(shard, axis, mask):
    pairs = [(i, i ^ mask) for i in range(lax.axis_size(axis))]
    return lax.ppermute(shard, axis, pairs)


def summary_join(earlier, latter):
    decay_first, peak_first, memory_first = earlier
    decay_second, peak_second, memory_second = latter
    peak_joined = jnp.maximum(decay_second + peak_first, peak_second)
    weight_first = jnp.exp(decay_second + peak_first - peak_joined)
    weight_second = jnp.exp(peak_second - peak_joined)
    return (
        decay_first + decay_second,
        peak_joined,
        weight_first * memory_first + weight_second * memory_second,
    )


def bits_of(size):
    assert size & (size - 1) == 0
    return size.bit_length() - 1


def from_xor_order(stacked, index, count):
    rest = stacked.shape[1:]
    bits = bits_of(count)
    for bit in range(bits):
        grid = stacked.reshape((count >> (bit + 1), 2, 1 << bit) + rest)
        flipped = jnp.concatenate([grid[:, 1:], grid[:, :1]], axis=1)
        stacked = jnp.where(((index >> bit) & 1) == 1, flipped, grid).reshape((count,) + rest)
    return stacked


def on_device(
    tokens,
    norm_gain,
    w_pool_in,
    w_mem_in,
    w_input_gate,
    w_forget_gate,
    forget_bias,
    forget_extra,
    conv_weight,
    query_map,
    key_map,
    pool_map,
    pool_gain,
    mem_gain,
    w_out_pool,
    w_out_mem,
):
    tp, sp = lax.axis_index("tp"), lax.axis_index("sp")
    n_tp, n_sp = lax.axis_size("tp"), lax.axis_size("sp")
    own_rows, width = tokens.shape
    heads = forget_extra.shape[1]
    parts = n_sp // heads
    slot, part = sp % heads, sp // heads
    head = tp * heads + slot
    depth, leave_cols = w_pool_in.shape[0], w_out_pool.shape[1]
    part_rows = own_rows * n_tp * heads
    blocks = part_rows // BLOCK
    both = 2 * HEAD

    normalized = rms_rows(tokens, norm_gain)
    sets = [jnp.stack([normalized] + [swap(normalized, "sp", k) for k in range(1, heads)])]
    for bit in reversed(range(bits_of(n_tp))):
        if bit == bits_of(n_tp) - 1:
            sets = sets + [swap(s, "tp", 1 << bit) for s in sets]
        else:
            sets = sets + [swap(s, "tp", 1 << bit) for s in sets]
    flips = [0]
    for bit in reversed(range(bits_of(n_tp))):
        flips = flips + [f | (1 << bit) for f in flips]
    by_flip = [sets[flips.index(f)] for f in range(n_tp)]

    def enter_block(of_slot):
        return jnp.concatenate(
            [
                lax.dynamic_slice_in_dim(w_pool_in, of_slot * HEAD, HEAD, 1),
                lax.dynamic_slice_in_dim(w_mem_in, of_slot * HEAD, HEAD, 1),
            ],
            axis=1,
        )

    def leave_block(of_slot):
        return jnp.concatenate(
            [
                lax.dynamic_slice_in_dim(w_out_pool, of_slot * HEAD, HEAD, 0),
                lax.dynamic_slice_in_dim(w_out_mem, of_slot * HEAD, HEAD, 0),
            ],
            axis=0,
        )

    gate_cols = jnp.concatenate(
        [
            lax.dynamic_slice_in_dim(w_input_gate, head, 1, 1),
            lax.dynamic_slice_in_dim(w_forget_gate, head, 1, 1),
            jnp.zeros((width, 126), bf16),
        ],
        axis=1,
    )
    enter = jnp.zeros((width, both), bf16)
    for k in range(n_sp):
        block = enter_block((sp ^ k) % heads)
        if k:
            block = swap(block, "sp", k)
        enter = lax.dynamic_update_slice(enter, block, ((sp ^ k) * depth, 0))
    leave_parts = []
    for k in range(n_sp):
        block = leave_block((sp ^ k) % heads)
        leave_parts.append(swap(block, "sp", k) if k else block)

    entered, gates = [], []
    gate_scale = jnp.where(jnp.arange(128) == 0, width ** (-0.5), 1.0).astype(f32)
    for rows in by_flip:
        rows = rows.reshape(heads * own_rows, width)
        entered.append(
            jnp.dot(rows, enter, preferred_element_type=f32)
            .astype(bf16)
            .reshape(heads, own_rows, both)
        )
        gates.append(
            (jnp.dot(rows, gate_cols, preferred_element_type=f32) * gate_scale)
            .astype(bf16)
            .reshape(heads, own_rows, 128)
        )

    def ordered(pieces):
        stacked = from_xor_order(jnp.stack(pieces), tp, n_tp)
        stacked = from_xor_order(jnp.swapaxes(stacked, 0, 1), slot, heads)
        return stacked.reshape(part_rows, -1)

    inputs = ordered(entered)
    gates = ordered(gates)[:, :2].astype(f32)
    input_pre = gates[:, 0].reshape(blocks, BLOCK)
    extra = [lax.dynamic_index_in_dim(forget_extra, slot, 1, False)]
    for k in range(1, heads):
        mine = lax.dynamic_index_in_dim(forget_extra, slot ^ k, 1, False)
        extra.append(swap(mine, "sp", k))
    extra = from_xor_order(jnp.stack(extra), slot, heads).reshape(part_rows)
    bias_own = lax.dynamic_slice_in_dim(forget_bias, head, 1, 0)
    log_forget = (jax.nn.log_sigmoid(gates[:, 1] + bias_own) - extra).reshape(blocks, BLOCK)

    input_blocks = inputs.reshape(blocks, BLOCK, both)
    rim = lax.ppermute(
        input_blocks[-1:], "sp", [(i, i + heads) for i in range(n_sp - heads)]
    )
    before = jnp.concatenate([rim, input_blocks[:-1]], axis=0)
    pair = jnp.concatenate([before, input_blocks], axis=1)
    lag = (jnp.arange(BLOCK)[:, None] + BLOCK) - jnp.arange(2 * BLOCK)[None, :]

    window = jnp.left_shift(2, head % 4)
    band = ((lag >= 0) & (lag < window)).astype(bf16)
    window_total = jnp.einsum(
        "ls,nsc->nlc", band, pair[:, :, :HEAD], preferred_element_type=f32
    )
    position = part * part_rows + jnp.arange(part_rows) + 1
    counts = jnp.minimum(position, window).astype(f32).reshape(blocks, BLOCK, 1)
    centred = (window_total / counts - input_blocks[:, :, :HEAD].astype(f32)).astype(bf16)
    own_map = lax.dynamic_index_in_dim(pool_map, slot, 0, False)
    pool_gain_own = lax.dynamic_slice_in_dim(pool_gain, head * HEAD, HEAD, 0).astype(f32)
    pool_mixed = (
        jnp.dot(centred.reshape(part_rows, HEAD), own_map, preferred_element_type=f32)
        * pool_gain_own
    ).astype(bf16)

    values = input_blocks[:, :, HEAD:]
    taps = lax.dynamic_slice_in_dim(conv_weight, head * HEAD, HEAD, 1).astype(f32)
    conv_sum = values.astype(f32) * taps[CONV - 1]
    for tap in range(CONV - 1):
        shift = (lag == CONV - 1 - tap).astype(bf16)
        moved = jnp.einsum("ls,nsc->nlc", shift, pair[:, :, HEAD:], preferred_element_type=f32)
        conv_sum = conv_sum + moved * taps[tap]
    conv_in = jax.nn.silu(conv_sum).astype(bf16).reshape(part_rows, HEAD)

    def dense_map(table):
        own = lax.dynamic_slice_in_dim(table, head * (HEAD // 4), HEAD // 4, 0).reshape(HEAD, 4)
        place = jnp.arange(HEAD) // 4
        return jnp.where(place[:, None] == place[None, :], jnp.tile(own, (1, HEAD // 4)), 0)

    def mapped(table):
        return (
            jnp.dot(conv_in, dense_map(table), preferred_element_type=f32)
            .astype(bf16)
            .reshape(blocks, BLOCK, HEAD)
        )

    query, keys = mapped(query_map), mapped(key_map)

    causal = jnp.tril(jnp.ones((BLOCK, BLOCK), dtype=jnp.bool_))
    cumulative = jnp.dot(log_forget, causal.astype(f32).T, precision=highest)
    total = cumulative[:, -1]
    along = total[:, None] - cumulative + input_pre
    along_peak = jnp.max(along, axis=-1)
    key_weight = jnp.exp(along - along_peak[:, None]) * HEAD ** (-0.5)
    scaled_keys = keys.astype(f32) * key_weight[..., None]
    block_memory = jnp.einsum("nld,nle->nde", scaled_keys, values.astype(f32), precision=highest)

    at = jnp.arange(blocks + 1)
    of = jnp.arange(blocks)
    between = (of[None, None, :] > of[None, :, None]) & (of[None, None, :] < at[:, None, None])
    log_left = jnp.sum(jnp.where(between, total, 0.0), axis=-1) + along_peak
    log_left = jnp.where(of[None, :] < at[:, None], log_left, -jnp.inf)
    peaks = jnp.maximum(jnp.max(log_left, axis=1), lowest)
    left = jnp.exp(log_left - peaks[:, None])
    memories = jnp.dot(left, block_memory.reshape(blocks, -1), precision=highest).reshape(
        blocks + 1, HEAD, HEAD
    )
    decays = jnp.sum(jnp.where(of[None, :] < at[:, None], total, 0.0), axis=-1)

    def from_before(state, by, fallback):
        pairs = [(i, i + by * heads) for i in range(n_sp - by * heads)]
        got = jax.tree.map(lambda a: lax.ppermute(a, "sp", pairs), state)
        return jax.tree.map(lambda a, b: jnp.where(part >= by, a, b), got, fallback)

    identity = (jnp.zeros((), f32), jnp.full((), lowest, f32), jnp.zeros((HEAD, HEAD), f32))
    state = (decays[-1], peaks[-1], memories[-1])
    state = from_before(state, 1, identity)
    by = 1
    while by < parts - 1:
        state = summary_join(from_before(state, by, identity), state)
        by *= 2
    in_decay, in_peak, in_memory = state
    start_peak = jnp.maximum(in_decay, in_peak)
    start_memory = jnp.exp(in_peak - start_peak) * in_memory
    block_peak = jnp.maximum(decays + start_peak, peaks)[:-1]
    block_state = (
        jnp.exp(decays[:-1] + start_peak - block_peak)[:, None, None] * start_memory
        + jnp.exp(peaks[:-1] - block_peak)[:, None, None] * memories[:-1]
    )

    log_diff = jnp.where(
        causal, cumulative[:, :, None] - cumulative[:, None, :] + input_pre[:, None, :], -jnp.inf
    )
    carry_log = cumulative + block_peak[:, None]
    row_peak = jnp.maximum(jnp.max(log_diff, axis=-1), carry_log)
    scores = jnp.einsum("nld,nsd->nls", query, keys, preferred_element_type=f32) * HEAD ** (-0.5)
    block_weights = (jnp.exp(log_diff - row_peak[..., None]) * scores).astype(bf16)
    within = jnp.einsum("nls,nse->nle", block_weights, values, preferred_element_type=f32)
    carried = jnp.einsum("nld,nde->nle", query.astype(f32), block_state, precision=highest)
    hidden = within + carried * jnp.exp(carry_log - row_peak)[..., None]
    centre = jnp.mean(hidden, axis=-1, keepdims=True)
    spread = jnp.mean(jnp.square(hidden - centre), axis=-1, keepdims=True)
    mem_gain_own = lax.dynamic_slice_in_dim(mem_gain, head * HEAD, HEAD, 0).astype(f32)
    mem_mixed = ((hidden - centre) * lax.rsqrt(spread + epsilon) * mem_gain_own).astype(bf16)
    mixed = jnp.concatenate([pool_mixed, mem_mixed.reshape(part_rows, HEAD)], axis=1)

    leave = jnp.zeros((both, width), bf16)
    for k in range(n_sp):
        leave = lax.dynamic_update_slice(leave, leave_parts[k], (0, (sp ^ k) * leave_cols))
    chunks = 2
    chunk_cols = width // chunks
    mine = (tp & 1) == 1
    by_core = mixed.reshape(heads, n_tp // 2, 2, own_rows, both)
    kept = jnp.where(mine, by_core[:, :, 1], by_core[:, :, 0])
    sent = jnp.where(mine, by_core[:, :, 0], by_core[:, :, 1])
    outs = []
    for chunk in range(chunks):
        weights = leave[:, chunk * chunk_cols : (chunk + 1) * chunk_cols]
        away = jnp.einsum("htrc,cd->htrd", sent, weights, preferred_element_type=f32)
        got = swap(away.astype(bf16), "tp", 1)
        held = jnp.einsum("htrc,cd->htrd", kept, weights, preferred_element_type=f32)
        held = (held.astype(bf16).astype(f32) + got.astype(f32)).astype(bf16)
        for bit in range(1, bits_of(n_tp)):
            halves = held.reshape(heads, -1, 2, own_rows, chunk_cols)
            on = (tp >> bit) & 1
            away = lax.dynamic_index_in_dim(halves, 1 - on, 2, False)
            got = swap(away, "tp", 1 << bit)
            held = lax.dynamic_index_in_dim(halves, on, 2, False)
            held = (held.astype(f32) + got.astype(f32)).astype(bf16)
        held = held.reshape(heads, own_rows, chunk_cols)
        result = lax.dynamic_index_in_dim(held, slot, 0, False).astype(f32)
        for k in range(1, heads):
            away = lax.dynamic_index_in_dim(held, slot ^ k, 0, False)
            result = result + swap(away, "sp", k).astype(f32)
        outs.append(result.astype(bf16))
    return jnp.concatenate(outs, axis=1)


def solution(mesh):
    placed = (
        P(("sp", "tp"), None),
        P(),
        P("sp", "tp"),
        P("sp", "tp"),
        P(),
        P(),
        P(),
        P("sp", "tp"),
        P(),
        P(),
        P(),
        P("tp", None, None),
        P(),
        P(),
        P("tp", "sp"),
        P("tp", "sp"),
    )
    return jax.shard_map(
        on_device, mesh=mesh, in_specs=placed, out_specs=P(("sp", "tp"), None), check_vma=False
    )
```

```python
import jax
import jax.numpy as jnp
from jax import lax
from jax.sharding import PartitionSpec as P

HEAD = 256
CONV = 4
BLOCK = 128

epsilon = 1e-06
highest = lax.Precision.HIGHEST
lowest = -1e30
f32 = jnp.float32
bf16 = jnp.bfloat16


def rms_rows(rows, gain):
    values = rows.astype(f32)
    factor = lax.rsqrt(jnp.mean(values * values, axis=-1, keepdims=True) + epsilon)
    return (values * factor * gain.astype(f32)).astype(bf16)


def swap(shard, axis, mask):
    pairs = [(i, i ^ mask) for i in range(lax.axis_size(axis))]
    return lax.ppermute(shard, axis, pairs)


def summary_join(earlier, latter):
    decay_first, peak_first, memory_first = earlier
    decay_second, peak_second, memory_second = latter
    peak_joined = jnp.maximum(decay_second + peak_first, peak_second)
    weight_first = jnp.exp(decay_second + peak_first - peak_joined)
    weight_second = jnp.exp(peak_second - peak_joined)
    return (
        decay_first + decay_second,
        peak_joined,
        weight_first * memory_first + weight_second * memory_second,
    )


def bits_of(size):
    assert size & (size - 1) == 0
    return size.bit_length() - 1


def from_xor_order(stacked, index, count):
    rest = stacked.shape[1:]
    bits = bits_of(count)
    for bit in range(bits):
        grid = stacked.reshape((count >> (bit + 1), 2, 1 << bit) + rest)
        flipped = jnp.concatenate([grid[:, 1:], grid[:, :1]], axis=1)
        stacked = jnp.where(((index >> bit) & 1) == 1, flipped, grid).reshape((count,) + rest)
    return stacked


def on_device(
    tokens,
    norm_gain,
    w_pool_in,
    w_mem_in,
    w_input_gate,
    w_forget_gate,
    forget_bias,
    forget_extra,
    conv_weight,
    query_map,
    key_map,
    pool_map,
    pool_gain,
    mem_gain,
    w_out_pool,
    w_out_mem,
):
    tp, sp = lax.axis_index("tp"), lax.axis_index("sp")
    n_tp, n_sp = lax.axis_size("tp"), lax.axis_size("sp")
    own_rows, width = tokens.shape
    heads = forget_extra.shape[1]
    parts = n_sp // heads
    slot, part = sp % heads, sp // heads
    head = tp * heads + slot
    depth, leave_cols = w_pool_in.shape[0], w_out_pool.shape[1]
    part_rows = own_rows * n_tp * heads
    blocks = part_rows // BLOCK
    both = 2 * HEAD

    normalized = rms_rows(tokens, norm_gain)
    pieces = [normalized] + [swap(normalized, "sp", k) for k in range(1, heads)]
    sets = [jnp.stack(pieces)]
    for bit in reversed(range(bits_of(n_tp))):
        if len(sets) == 1:
            sets = sets + [jnp.stack([swap(p, "tp", 1 << bit) for p in pieces])]
        else:
            sets = sets + [swap(s, "tp", 1 << bit) for s in sets]
    flips = [0]
    for bit in reversed(range(bits_of(n_tp))):
        flips = flips + [f | (1 << bit) for f in flips]
    by_flip = [sets[flips.index(f)] for f in range(n_tp)]

    def enter_block(of_slot):
        return jnp.concatenate(
            [
                lax.dynamic_slice_in_dim(w_pool_in, of_slot * HEAD, HEAD, 1),
                lax.dynamic_slice_in_dim(w_mem_in, of_slot * HEAD, HEAD, 1),
            ],
            axis=1,
        )

    def leave_block(of_slot):
        return jnp.concatenate(
            [
                lax.dynamic_slice_in_dim(w_out_pool, of_slot * HEAD, HEAD, 0),
                lax.dynamic_slice_in_dim(w_out_mem, of_slot * HEAD, HEAD, 0),
            ],
            axis=0,
        )

    gate_cols = jnp.concatenate(
        [
            lax.dynamic_slice_in_dim(w_input_gate, head, 1, 1),
            lax.dynamic_slice_in_dim(w_forget_gate, head, 1, 1),
            jnp.zeros((width, 126), bf16),
        ],
        axis=1,
    )
    enter_parts = []
    for k in range(n_sp):
        block = enter_block((sp ^ k) % heads)
        enter_parts.append(swap(block, "sp", k) if k else block)
    leave_parts = []
    for k in range(n_sp):
        block = leave_block((sp ^ k) % heads)
        leave_parts.append(swap(block, "sp", k) if k else block)
    enter_parts[1], forget_extra = lax.optimization_barrier((enter_parts[1], forget_extra))
    enter = jnp.concatenate([jnp.zeros((width, both), bf16), gate_cols], axis=1)
    for k in range(n_sp):
        enter = lax.dynamic_update_slice(enter, enter_parts[k], ((sp ^ k) * depth, 0))

    column_scale = jnp.where(jnp.arange(both + 128) == both, width ** (-0.5), 1.0).astype(f32)
    entered = [
        (
            jnp.dot(rows.reshape(heads * own_rows, width), enter, preferred_element_type=f32)
            * column_scale
        )
        .astype(bf16)
        .reshape(heads, own_rows, both + 128)
        for rows in by_flip
    ]

    def ordered(pieces):
        stacked = from_xor_order(jnp.stack(pieces), tp, n_tp)
        stacked = from_xor_order(jnp.swapaxes(stacked, 0, 1), slot, heads)
        return stacked.reshape(part_rows, -1)

    inputs_gates = ordered(entered)
    inputs = inputs_gates[:, :both]
    gates = inputs_gates[:, both : both + 2].astype(f32)
    input_pre = gates[:, 0].reshape(blocks, BLOCK)
    extra = [lax.dynamic_index_in_dim(forget_extra, slot, 1, False)]
    for k in range(1, heads):
        mine = lax.dynamic_index_in_dim(forget_extra, slot ^ k, 1, False)
        extra.append(swap(mine, "sp", k))
    extra = from_xor_order(jnp.stack(extra), slot, heads).reshape(part_rows)
    bias_own = lax.dynamic_slice_in_dim(forget_bias, head, 1, 0)
    log_forget = (jax.nn.log_sigmoid(gates[:, 1] + bias_own) - extra).reshape(blocks, BLOCK)

    input_blocks = inputs.reshape(blocks, BLOCK, both)
    rim = lax.ppermute(
        input_blocks[-1:], "sp", [(i, i + heads) for i in range(n_sp - heads)]
    )
    before = jnp.concatenate([rim, input_blocks[:-1]], axis=0)
    pair = jnp.concatenate([before, input_blocks], axis=1)
    lag = (jnp.arange(BLOCK)[:, None] + BLOCK) - jnp.arange(2 * BLOCK)[None, :]

    window = jnp.left_shift(2, head % 4)
    band = ((lag >= 0) & (lag < window)).astype(bf16)
    window_total = jnp.einsum(
        "ls,nsc->nlc", band, pair[:, :, :HEAD], preferred_element_type=f32
    )
    position = part * part_rows + jnp.arange(part_rows) + 1
    counts = jnp.minimum(position, window).astype(f32).reshape(blocks, BLOCK, 1)
    centred = (window_total / counts - input_blocks[:, :, :HEAD].astype(f32)).astype(bf16)
    own_map = lax.dynamic_index_in_dim(pool_map, slot, 0, False)
    pool_gain_own = lax.dynamic_slice_in_dim(pool_gain, head * HEAD, HEAD, 0).astype(f32)
    pool_mixed = (
        jnp.dot(centred.reshape(part_rows, HEAD), own_map, preferred_element_type=f32)
        * pool_gain_own
    ).astype(bf16)

    values = input_blocks[:, :, HEAD:]
    taps = lax.dynamic_slice_in_dim(conv_weight, head * HEAD, HEAD, 1).astype(f32)
    conv_sum = values.astype(f32) * taps[CONV - 1]
    for tap in range(CONV - 1):
        shift = (lag == CONV - 1 - tap).astype(bf16)
        moved = jnp.einsum("ls,nsc->nlc", shift, pair[:, :, HEAD:], preferred_element_type=f32)
        conv_sum = conv_sum + moved * taps[tap]
    conv_in = jax.nn.silu(conv_sum).astype(bf16).reshape(part_rows, HEAD)

    def dense_map(table):
        own = lax.dynamic_slice_in_dim(table, head * (HEAD // 4), HEAD // 4, 0).reshape(HEAD, 4)
        place = jnp.arange(HEAD) // 4
        return jnp.where(place[:, None] == place[None, :], jnp.tile(own, (1, HEAD // 4)), 0)

    def mapped(table):
        return (
            jnp.dot(conv_in, dense_map(table), preferred_element_type=f32)
            .astype(bf16)
            .reshape(blocks, BLOCK, HEAD)
        )

    query, keys = mapped(query_map), mapped(key_map)

    causal = jnp.tril(jnp.ones((BLOCK, BLOCK), dtype=jnp.bool_))
    cumulative = jnp.dot(log_forget, causal.astype(f32).T, precision=highest)
    total = cumulative[:, -1]
    along = total[:, None] - cumulative + input_pre
    along_peak = jnp.max(along, axis=-1)
    key_weight = jnp.exp(along - along_peak[:, None]) * HEAD ** (-0.5)
    scaled_keys = keys.astype(f32) * key_weight[..., None]
    block_memory = jnp.einsum("nld,nle->nde", scaled_keys, values.astype(f32), precision=highest)

    at = jnp.arange(blocks + 1)
    of = jnp.arange(blocks)
    between = (of[None, None, :] > of[None, :, None]) & (of[None, None, :] < at[:, None, None])
    log_left = jnp.sum(jnp.where(between, total, 0.0), axis=-1) + along_peak
    log_left = jnp.where(of[None, :] < at[:, None], log_left, -jnp.inf)
    peaks = jnp.maximum(jnp.max(log_left, axis=1), lowest)
    left = jnp.exp(log_left - peaks[:, None])
    memories = jnp.dot(left, block_memory.reshape(blocks, -1), precision=highest).reshape(
        blocks + 1, HEAD, HEAD
    )
    decays = jnp.sum(jnp.where(of[None, :] < at[:, None], total, 0.0), axis=-1)

    def from_before(state, by, fallback):
        pairs = [(i, i + by * heads) for i in range(n_sp - by * heads)]
        decay, peak, memory = state
        packed = jnp.concatenate(
            [memory, jnp.full((4, HEAD), decay, f32), jnp.full((4, HEAD), peak, f32)], axis=0
        )
        packed = lax.ppermute(packed, "sp", pairs)
        got = packed[HEAD, 0], packed[HEAD + 4, 0], packed[:HEAD]
        return jax.tree.map(lambda a, b: jnp.where(part >= by, a, b), got, fallback)

    identity = (jnp.zeros((), f32), jnp.full((), lowest, f32), jnp.zeros((HEAD, HEAD), f32))
    state = (decays[-1], peaks[-1], memories[-1])
    state = from_before(state, 1, identity)
    by = 1
    while by < parts - 1:
        state = summary_join(from_before(state, by, identity), state)
        by *= 2
    in_decay, in_peak, in_memory = state
    start_peak = jnp.maximum(in_decay, in_peak)
    start_memory = jnp.exp(in_peak - start_peak) * in_memory
    block_peak = jnp.maximum(decays + start_peak, peaks)[:-1]
    block_state = (
        jnp.exp(decays[:-1] + start_peak - block_peak)[:, None, None] * start_memory
        + jnp.exp(peaks[:-1] - block_peak)[:, None, None] * memories[:-1]
    )

    log_diff = jnp.where(
        causal, cumulative[:, :, None] - cumulative[:, None, :] + input_pre[:, None, :], -jnp.inf
    )
    carry_log = cumulative + block_peak[:, None]
    row_peak = jnp.maximum(jnp.max(log_diff, axis=-1), carry_log)
    scores = jnp.einsum("nld,nsd->nls", query, keys, preferred_element_type=f32) * HEAD ** (-0.5)
    block_weights = (jnp.exp(log_diff - row_peak[..., None]) * scores).astype(bf16)
    within = jnp.einsum("nls,nse->nle", block_weights, values, preferred_element_type=f32)
    carried = jnp.einsum("nld,nde->nle", query.astype(f32), block_state, precision=highest)
    hidden = within + carried * jnp.exp(carry_log - row_peak)[..., None]
    centre = jnp.mean(hidden, axis=-1, keepdims=True)
    spread = jnp.mean(jnp.square(hidden - centre), axis=-1, keepdims=True)
    mem_gain_own = lax.dynamic_slice_in_dim(mem_gain, head * HEAD, HEAD, 0).astype(f32)
    mem_mixed = ((hidden - centre) * lax.rsqrt(spread + epsilon) * mem_gain_own).astype(bf16)
    mixed = jnp.concatenate([pool_mixed, mem_mixed.reshape(part_rows, HEAD)], axis=1)

    leave_parts, mixed = lax.optimization_barrier((leave_parts, mixed))
    mine = (tp & 1) == 1
    by_core = mixed.reshape(heads, n_tp // 2, 2, own_rows, both)
    kept = jnp.where(mine, by_core[:, :, 1], by_core[:, :, 0])
    sent = jnp.where(mine, by_core[:, :, 0], by_core[:, :, 1])
    group_cols = heads * leave_cols

    def over_tp(held):
        for bit in range(1, bits_of(n_tp)):
            halves = held.reshape(held.shape[0], -1, 2, own_rows, group_cols)
            on = (tp >> bit) & 1
            got = swap(lax.dynamic_index_in_dim(halves, 1 - on, 2, False), "tp", 1 << bit)
            held = lax.dynamic_index_in_dim(halves, on, 2, False)
            held = (held.astype(f32) + got.astype(f32)).astype(bf16)
        return held

    def over_slots(held):
        result = lax.dynamic_index_in_dim(held, slot, 0, True).astype(f32)
        for k in range(1, heads):
            got = swap(lax.dynamic_index_in_dim(held, slot ^ k, 0, True), "sp", k)
            got = jnp.concatenate(
                [got[..., (c ^ k) * leave_cols :][..., :leave_cols] for c in range(heads)], axis=-1
            )
            result = result + got.astype(f32)
        return result.astype(bf16)

    outs = []
    for group in range(parts):
        weights = jnp.concatenate(leave_parts[group * heads : (group + 1) * heads], axis=1)
        away = jnp.einsum("htrc,cd->htrd", sent, weights, preferred_element_type=f32)
        got = swap(away.astype(bf16), "tp", 1)
        held = jnp.einsum("htrc,cd->htrd", kept, weights, preferred_element_type=f32)
        held = (held.astype(bf16).astype(f32) + got.astype(f32)).astype(bf16)
        result = over_slots(over_tp(held)) if group % 2 == 0 else over_tp(over_slots(held))
        outs.append(result.reshape(own_rows, group_cols))
    result = jnp.concatenate(outs, axis=1)
    for bit in range(bits_of(n_sp)):
        blocks_now = [result[:, c * leave_cols : (c + 1) * leave_cols] for c in range(n_sp)]
        flipped = jnp.concatenate([blocks_now[c ^ (1 << bit)] for c in range(n_sp)], axis=1)
        result = jnp.where(((sp >> bit) & 1) == 1, flipped, result)
    return result


def solution(mesh):
    placed = (
        P(("sp", "tp"), None),
        P(),
        P("sp", "tp"),
        P("sp", "tp"),
        P(),
        P(),
        P(),
        P("sp", "tp"),
        P(),
        P(),
        P(),
        P("tp", None, None),
        P(),
        P(),
        P("tp", "sp"),
        P("tp", "sp"),
    )
    return jax.shard_map(
        on_device, mesh=mesh, in_specs=placed, out_specs=P(("sp", "tp"), None), check_vma=False
    )
```

```python
import jax
import jax.numpy as jnp
from jax import lax
from jax.sharding import PartitionSpec as P

HEAD = 256
CONV = 4
BLOCK = 128

epsilon = 1e-06
highest = lax.Precision.HIGHEST
lowest = -1e30
f32 = jnp.float32
bf16 = jnp.bfloat16


def rms_rows(rows, gain):
    values = rows.astype(f32)
    factor = lax.rsqrt(jnp.mean(values * values, axis=-1, keepdims=True) + epsilon)
    return (values * factor * gain.astype(f32)).astype(bf16)


def swap(shard, axis, mask):
    pairs = [(i, i ^ mask) for i in range(lax.axis_size(axis))]
    return lax.ppermute(shard, axis, pairs)


def summary_join(earlier, latter):
    decay_first, peak_first, memory_first = earlier
    decay_second, peak_second, memory_second = latter
    peak_joined = jnp.maximum(decay_second + peak_first, peak_second)
    weight_first = jnp.exp(decay_second + peak_first - peak_joined)
    weight_second = jnp.exp(peak_second - peak_joined)
    return (
        decay_first + decay_second,
        peak_joined,
        weight_first * memory_first + weight_second * memory_second,
    )


def bits_of(size):
    assert size & (size - 1) == 0
    return size.bit_length() - 1


def from_xor_order(stacked, index, count):
    rest = stacked.shape[1:]
    bits = bits_of(count)
    for bit in range(bits):
        grid = stacked.reshape((count >> (bit + 1), 2, 1 << bit) + rest)
        flipped = jnp.concatenate([grid[:, 1:], grid[:, :1]], axis=1)
        stacked = jnp.where(((index >> bit) & 1) == 1, flipped, grid).reshape((count,) + rest)
    return stacked


def on_device(
    tokens,
    norm_gain,
    w_pool_in,
    w_mem_in,
    w_input_gate,
    w_forget_gate,
    forget_bias,
    forget_extra,
    conv_weight,
    query_map,
    key_map,
    pool_map,
    pool_gain,
    mem_gain,
    w_out_pool,
    w_out_mem,
):
    tp, sp = lax.axis_index("tp"), lax.axis_index("sp")
    n_tp, n_sp = lax.axis_size("tp"), lax.axis_size("sp")
    own_rows, width = tokens.shape
    heads = forget_extra.shape[1]
    parts = n_sp // heads
    slot, part = sp % heads, sp // heads
    head = tp * heads + slot
    depth, leave_cols = w_pool_in.shape[0], w_out_pool.shape[1]
    part_rows = own_rows * n_tp * heads
    blocks = part_rows // BLOCK
    both = 2 * HEAD

    normalized = rms_rows(tokens, norm_gain)
    pieces = [normalized] + [swap(normalized, "sp", k) for k in range(1, heads)]
    coarse = 1 << (bits_of(n_tp) - 1)
    early = [swap(p, "tp", coarse) for p in pieces]

    def enter_block(of_slot):
        return jnp.concatenate(
            [
                lax.dynamic_slice_in_dim(w_pool_in, of_slot * HEAD, HEAD, 1),
                lax.dynamic_slice_in_dim(w_mem_in, of_slot * HEAD, HEAD, 1),
            ],
            axis=1,
        )

    def leave_block(of_slot, pool_now, mem_now):
        return jnp.concatenate(
            [
                lax.dynamic_slice_in_dim(pool_now, of_slot * HEAD, HEAD, 0),
                lax.dynamic_slice_in_dim(mem_now, of_slot * HEAD, HEAD, 0),
            ],
            axis=0,
        )

    gate_cols = jnp.concatenate(
        [
            lax.dynamic_slice_in_dim(w_input_gate, head, 1, 1),
            lax.dynamic_slice_in_dim(w_forget_gate, head, 1, 1),
            jnp.zeros((width, 126), bf16),
        ],
        axis=1,
    )
    enter_parts = [None] * n_sp
    for k in list(range(heads, n_sp)) + list(range(heads)):
        block = enter_block((sp ^ k) % heads)
        enter_parts[k] = swap(block, "sp", k) if k else block

    leave_parts = [None] * n_sp
    first_batch, second_batch = n_sp - n_sp // 4, n_sp - n_sp // 8
    def send_leave(first, last, behind):
        behind, pool_now, mem_now = lax.optimization_barrier((behind, w_out_pool, w_out_mem))
        for k in sorted(range(first, last), reverse=True):
            block = leave_block((sp ^ k) % heads, pool_now, mem_now)
            leave_parts[k] = swap(block, "sp", k) if k else block
        return behind

    forget_extra = lax.optimization_barrier((forget_extra, *pieces))[0]
    extra = [lax.dynamic_index_in_dim(forget_extra, slot, 1, False)]
    for k in range(1, heads):
        mine = lax.dynamic_index_in_dim(forget_extra, slot ^ k, 1, False)
        extra.append(swap(mine, "sp", k))
    extra = from_xor_order(jnp.stack(extra), slot, heads).reshape(part_rows)
    extra = send_leave(0, first_batch, extra)
    extra, *enter_parts = lax.optimization_barrier((extra, *enter_parts))
    sets, flips = [jnp.stack(pieces), jnp.stack(early)], [0, coarse]
    for bit in reversed(range(bits_of(n_tp) - 1)):
        sets = sets + [swap(held, "tp", 1 << bit) for held in sets]
        flips = flips + [flip | (1 << bit) for flip in flips]
    by_flip = [sets[flips.index(flip)] for flip in range(n_tp)]

    enter = jnp.concatenate([jnp.zeros((width, both), bf16), gate_cols], axis=1)
    for k in range(n_sp):
        enter = lax.dynamic_update_slice(enter, enter_parts[k], ((sp ^ k) * depth, 0))

    column_scale = jnp.where(jnp.arange(both + 128) == both, width ** (-0.5), 1.0).astype(f32)
    entered = [
        (
            jnp.dot(rows.reshape(heads * own_rows, width), enter, preferred_element_type=f32)
            * column_scale
        )
        .astype(bf16)
        .reshape(heads, own_rows, both + 128)
        for rows in by_flip
    ]

    def ordered(pieces):
        stacked = from_xor_order(jnp.stack(pieces), tp, n_tp)
        stacked = from_xor_order(jnp.swapaxes(stacked, 0, 1), slot, heads)
        return stacked.reshape(part_rows, -1)

    inputs_gates = ordered(entered)
    inputs = inputs_gates[:, :both]
    gates = inputs_gates[:, both : both + 2].astype(f32)
    input_pre = gates[:, 0].reshape(blocks, BLOCK)
    bias_own = lax.dynamic_slice_in_dim(forget_bias, head, 1, 0)
    log_forget = (jax.nn.log_sigmoid(gates[:, 1] + bias_own) - extra).reshape(blocks, BLOCK)

    input_blocks = inputs.reshape(blocks, BLOCK, both)
    rim = lax.ppermute(
        input_blocks[-1:], "sp", [(i, i + heads) for i in range(n_sp - heads)]
    )
    rim = send_leave(first_batch, second_batch, rim)
    before = jnp.concatenate([rim, input_blocks[:-1]], axis=0)
    pair = jnp.concatenate([before, input_blocks], axis=1)
    lag = (jnp.arange(BLOCK)[:, None] + BLOCK) - jnp.arange(2 * BLOCK)[None, :]

    window = jnp.left_shift(2, head % 4)
    band = ((lag >= 0) & (lag < window)).astype(bf16)
    window_total = jnp.einsum(
        "ls,nsc->nlc", band, pair[:, :, :HEAD], preferred_element_type=f32
    )
    position = part * part_rows + jnp.arange(part_rows) + 1
    counts = jnp.minimum(position, window).astype(f32).reshape(blocks, BLOCK, 1)
    centred = (window_total / counts - input_blocks[:, :, :HEAD].astype(f32)).astype(bf16)
    own_map = lax.dynamic_index_in_dim(pool_map, slot, 0, False)
    pool_gain_own = lax.dynamic_slice_in_dim(pool_gain, head * HEAD, HEAD, 0).astype(f32)
    pool_mixed = (
        jnp.dot(centred.reshape(part_rows, HEAD), own_map, preferred_element_type=f32)
        * pool_gain_own
    ).astype(bf16)

    values = input_blocks[:, :, HEAD:]
    taps = lax.dynamic_slice_in_dim(conv_weight, head * HEAD, HEAD, 1).astype(f32)
    conv_sum = values.astype(f32) * taps[CONV - 1]
    for tap in range(CONV - 1):
        shift = (lag == CONV - 1 - tap).astype(bf16)
        moved = jnp.einsum("ls,nsc->nlc", shift, pair[:, :, HEAD:], preferred_element_type=f32)
        conv_sum = conv_sum + moved * taps[tap]
    conv_in = jax.nn.silu(conv_sum).astype(bf16).reshape(part_rows, HEAD)

    def dense_map(table):
        own = lax.dynamic_slice_in_dim(table, head * (HEAD // 4), HEAD // 4, 0).reshape(HEAD, 4)
        place = jnp.arange(HEAD) // 4
        return jnp.where(place[:, None] == place[None, :], jnp.tile(own, (1, HEAD // 4)), 0)

    def mapped(table):
        return (
            jnp.dot(conv_in, dense_map(table), preferred_element_type=f32)
            .astype(bf16)
            .reshape(blocks, BLOCK, HEAD)
        )

    query, keys = mapped(query_map), mapped(key_map)

    causal = jnp.tril(jnp.ones((BLOCK, BLOCK), dtype=jnp.bool_))
    cumulative = jnp.dot(log_forget, causal.astype(f32).T, precision=highest)
    total = cumulative[:, -1]
    along = total[:, None] - cumulative + input_pre
    along_peak = jnp.max(along, axis=-1)
    key_weight = jnp.exp(along - along_peak[:, None]) * HEAD ** (-0.5)
    scaled_keys = keys.astype(f32) * key_weight[..., None]
    block_memory = jnp.einsum("nld,nle->nde", scaled_keys, values.astype(f32), precision=highest)

    at = jnp.arange(blocks + 1)
    of = jnp.arange(blocks)
    between = (of[None, None, :] > of[None, :, None]) & (of[None, None, :] < at[:, None, None])
    log_left = jnp.sum(jnp.where(between, total, 0.0), axis=-1) + along_peak
    log_left = jnp.where(of[None, :] < at[:, None], log_left, -jnp.inf)
    peaks = jnp.maximum(jnp.max(log_left, axis=1), lowest)
    left = jnp.exp(log_left - peaks[:, None])
    memories = jnp.dot(left, block_memory.reshape(blocks, -1), precision=highest).reshape(
        blocks + 1, HEAD, HEAD
    )
    decays = jnp.sum(jnp.where(of[None, :] < at[:, None], total, 0.0), axis=-1)

    def from_before(state, by, fallback):
        pairs = [(i, i + by * heads) for i in range(n_sp - by * heads)]
        decay, peak, memory = state
        packed = jnp.concatenate(
            [memory, jnp.full((4, HEAD), decay, f32), jnp.full((4, HEAD), peak, f32)], axis=0
        )
        packed = lax.ppermute(packed, "sp", pairs)
        got = packed[HEAD, 0], packed[HEAD + 4, 0], packed[:HEAD]
        return jax.tree.map(lambda a, b: jnp.where(part >= by, a, b), got, fallback)

    identity = (jnp.zeros((), f32), jnp.full((), lowest, f32), jnp.zeros((HEAD, HEAD), f32))
    state = (decays[-1], peaks[-1], memories[-1])
    state = from_before(state, 1, identity)
    by = 1
    while by < parts - 1:
        state = summary_join(from_before(state, by, identity), state)
        by *= 2
    in_decay, in_peak, in_memory = state
    in_memory = send_leave(second_batch, n_sp, in_memory)
    start_peak = jnp.maximum(in_decay, in_peak)
    start_memory = jnp.exp(in_peak - start_peak) * in_memory
    block_peak = jnp.maximum(decays + start_peak, peaks)[:-1]
    block_state = (
        jnp.exp(decays[:-1] + start_peak - block_peak)[:, None, None] * start_memory
        + jnp.exp(peaks[:-1] - block_peak)[:, None, None] * memories[:-1]
    )

    log_diff = jnp.where(
        causal, cumulative[:, :, None] - cumulative[:, None, :] + input_pre[:, None, :], -jnp.inf
    )
    carry_log = cumulative + block_peak[:, None]
    row_peak = jnp.maximum(jnp.max(log_diff, axis=-1), carry_log)
    scores = jnp.einsum("nld,nsd->nls", query, keys, preferred_element_type=f32) * HEAD ** (-0.5)
    block_weights = (jnp.exp(log_diff - row_peak[..., None]) * scores).astype(bf16)
    within = jnp.einsum("nls,nse->nle", block_weights, values, preferred_element_type=f32)
    carried = jnp.einsum("nld,nde->nle", query.astype(f32), block_state, precision=highest)
    hidden = within + carried * jnp.exp(carry_log - row_peak)[..., None]
    centre = jnp.mean(hidden, axis=-1, keepdims=True)
    spread = jnp.mean(jnp.square(hidden - centre), axis=-1, keepdims=True)
    mem_gain_own = lax.dynamic_slice_in_dim(mem_gain, head * HEAD, HEAD, 0).astype(f32)
    mem_mixed = ((hidden - centre) * lax.rsqrt(spread + epsilon) * mem_gain_own).astype(bf16)
    mixed = jnp.concatenate([pool_mixed, mem_mixed.reshape(part_rows, HEAD)], axis=1)

    leave_parts, mixed = lax.optimization_barrier((leave_parts, mixed))
    mine = (tp & 1) == 1
    by_core = mixed.reshape(heads, n_tp // 2, 2, own_rows, both)
    kept = jnp.where(mine, by_core[:, :, 1], by_core[:, :, 0]).reshape(-1, both)
    sent = jnp.where(mine, by_core[:, :, 0], by_core[:, :, 1]).reshape(-1, both)
    group_cols = heads * leave_cols

    def over_tp(held):
        for bit in range(1, bits_of(n_tp)):
            halves = held.reshape(held.shape[0], -1, 2, own_rows, group_cols)
            on = (tp >> bit) & 1
            got = swap(lax.dynamic_index_in_dim(halves, 1 - on, 2, False), "tp", 1 << bit)
            held = lax.dynamic_index_in_dim(halves, on, 2, False)
            held = (held.astype(f32) + got.astype(f32)).astype(bf16)
        return held

    def over_slots(held):
        result = lax.dynamic_index_in_dim(held, slot, 0, True).astype(f32)
        for k in range(1, heads):
            got = swap(lax.dynamic_index_in_dim(held, slot ^ k, 0, True), "sp", k)
            got = jnp.concatenate(
                [got[..., (c ^ k) * leave_cols :][..., :leave_cols] for c in range(heads)], axis=-1
            )
            result = result + got.astype(f32)
        return result.astype(bf16)

    outs = []
    for group in range(parts):
        weights = jnp.concatenate(leave_parts[group * heads : (group + 1) * heads], axis=1)
        away = jnp.dot(sent, weights, preferred_element_type=f32).astype(bf16)
        got = swap(away, "tp", 1)
        held = jnp.dot(kept, weights, preferred_element_type=f32).astype(bf16)
        held = (held.astype(f32) + got.astype(f32)).astype(bf16)
        held = held.reshape(heads, n_tp // 2, own_rows, group_cols)
        result = over_slots(over_tp(held)) if group % 2 == 0 else over_tp(over_slots(held))
        outs.append(result.reshape(own_rows, group_cols))
    result = jnp.concatenate(outs, axis=1)
    for bit in range(bits_of(n_sp)):
        blocks_now = [result[:, c * leave_cols : (c + 1) * leave_cols] for c in range(n_sp)]
        flipped = jnp.concatenate([blocks_now[c ^ (1 << bit)] for c in range(n_sp)], axis=1)
        result = jnp.where(((sp >> bit) & 1) == 1, flipped, result)
    return result


def solution(mesh):
    placed = (
        P(("sp", "tp"), None),
        P(),
        P("sp", "tp"),
        P("sp", "tp"),
        P(),
        P(),
        P(),
        P("sp", "tp"),
        P(),
        P(),
        P(),
        P("tp", None, None),
        P(),
        P(),
        P("tp", "sp"),
        P("tp", "sp"),
    )
    return jax.shard_map(
        on_device, mesh=mesh, in_specs=placed, out_specs=P(("sp", "tp"), None), check_vma=False
    )
```
